128 devices in a mesh: ep: 32 (over z, y, core), tp: 4 (over x).
Axes of the slice: x: 4, y: 4, z: 4, core: 2. Of those that a mesh axis runs over, the one named last changes fastest.
Arguments:
- queries: bfloat16 [16384, 1024], P('ep', 'tp'), may hold values from -10.5 to 10.5
- keys: bfloat16 [16384, 512], P('ep', 'tp'), may hold values from -10.5 to 10.5
- values: bfloat16 [16384, 512], P('ep', 'tp'), may hold values from -6 to 6
- head_lambda: float32 [8], P('tp'), may hold values from 0.3 to 0.8
- out_gain: float32 [128], replicated, may hold values from 0.1 to 1.9
- expert_input: bfloat16 [16384, 2048], P(('ep', 'tp')), may hold values from -6 to 6
- routes: int32 [16384, 4], P(('ep', 'tp')), may hold values from 0 to 31, all different within a row; in each aligned block of 128 rows (0 to 127, 128 to 255, ...) at most 20 rows name the same one
- route_weight: float32 [16384, 4], P(('ep', 'tp')), may hold values from 0.2 to 0.6
- moe_gain: float32 [2048], replicated, may hold values from 0.1 to 1.9
- gate_weight: bfloat16 [32, 2048, 2048], P('ep', None, 'tp'), may hold values from -0.3125 to 0.3125
- up_weight: bfloat16 [32, 2048, 2048], P('ep', None, 'tp'), may hold values from -0.3125 to 0.3125
- down_weight: bfloat16 [32, 2048, 2048], P('ep', 'tp'), may hold values from -0.03125 to 0.03125
Outputs:
- mixed_out: bfloat16 [16384, 1024], P('ep', 'tp')
- expert_mix: bfloat16 [16384, 2048], P(('ep', 'tp'))
The draws below stay inside these ranges and needn't reach their ends.
Inputs may be any that keep to these rules, and one draw needn't show every extreme that they name: `routes`: each row names 4 different experts. Among the rows of one device (aligned blocks of 128 rows) no expert is named more than 20 times, and in some blocks one is named exactly 20 times.
All inputs are finite; a program needn't handle non-finite values.
Results may differ from the reference program's by a relative error of at most 0.012.
Values may be sent and summed in bfloat16 or wider, within the bound.
No kernel may reach another device: no remote copies, remote signals or barrier semaphores. Data moves between devices by JAX's collectives and lax.ppermute only.
A program may use at most 128 MiB of HBM per device.

```python
import math
import jax
import jax.numpy as jnp
import numpy as np
from jax import lax

D = 2048
HEADS = 8
KV_HEADS = 4
HEAD = 64
VDIM = 128
FF = 2048
TOPK = 4
TOK_DEV = 128
LEN = 16384
TOKENS = 16384
EXPERTS = 32
CAP = 20
N_EP = 32
N_TP = 4


def draw_queries(key, part):
    folded = jax.random.fold_in(key, 101)
    drawn_field = jnp.clip(jax.random.normal(folded, (LEN, HEADS, 2, HEAD), jnp.float32) * 1.32, -7.9, 7.9)
    return drawn_field.reshape(LEN, HEADS * 2 * HEAD).astype(jnp.bfloat16)


def draw_keys(key, part):
    folded = jax.random.fold_in(key, 202)
    drawn_field = jnp.clip(jax.random.normal(folded, (LEN, KV_HEADS, 2, HEAD), jnp.float32) * 1.32, -7.9, 7.9)
    return drawn_field.reshape(LEN, KV_HEADS * 2 * HEAD).astype(jnp.bfloat16)


def block_scale(stream_key, extent, cuts, least, largest):
    gain = 1.0
    for axis_at, shards_of in cuts:
        draws = jax.random.uniform(jax.random.fold_in(jax.random.fold_in(stream_key, 6), axis_at), (shards_of,), jnp.float32, least / len(cuts), largest / len(cuts))
        gain = gain * jnp.repeat(jnp.exp(draws), extent[axis_at] // shards_of).reshape((-1,) + (1,) * (len(extent) - 1 - axis_at))
    return gain


def assign_block(stream_key, own, number, rows, count, top, most, skew):
    order = jax.random.permutation(stream_key, count)
    crowded, ordinary = load_shares(count, rows * top, most, skew, True), load_shares(count, rows * top, most, skew, False)
    places = jnp.arange(count)

    def named(tallies, rotation):
        used = int((tallies > 0).sum())
        fixed = max(1, used // 4)
        moved = fixed + (places - fixed + rotation * (used - fixed)) % max(1, count - fixed)
        return jnp.zeros((count,), jnp.int32).at[order[jnp.where(places < fixed, places, moved)]].set(jnp.asarray(tallies, jnp.int32))

    tallies = jnp.where(number % 4 == 0, named(crowded, number // 4), named(ordinary, number - number // 4 - 1))
    mixed = jax.random.permutation(jax.random.fold_in(own, 3), count)
    donor, receiver = mixed[0:count // 2 * 2:2], mixed[1:count // 2 * 2:2]
    margin = jnp.minimum(tallies[donor] - 1, most - tallies[receiver]) // 2
    margin = jnp.where((donor == order[0]) | (receiver == order[0]) | (tallies[receiver] == 0), 0, jnp.maximum(margin, 0))
    moved = jax.random.randint(jax.random.fold_in(own, 4), (count // 2,), 0, 1 << 20) % (margin + 1)
    tallies = tallies.at[donor].add(-moved).at[receiver].add(moved)
    items = jnp.searchsorted(jnp.cumsum(tallies), jnp.arange(rows * top), side="right").astype(jnp.int32)
    listing = items.reshape(top, rows).T
    listing = listing[jax.random.permutation(jax.random.fold_in(own, 1), rows)]
    rotation = jax.random.randint(jax.random.fold_in(own, 2), (rows, 1), 0, top)
    return jnp.take_along_axis(listing, (jnp.arange(top)[None, :] + rotation) % top, axis=1)


def load_shares(amount, total, most, lean, full):
    loads = [(1 << 20) // math.isqrt(standing ** lean) + 1 for standing in range(1, amount + 1)]
    largest = most if full else min(most, max(-(-total // amount), total * loads[0] // sum(loads)))
    least = 1 if total - largest >= amount - 1 else 0
    given, rest = [largest] + [least] * (amount - 1), total - largest - least * (amount - 1)
    while rest > 0:
        movable = [i for i in range(1, amount) if given[i] < largest] or [i for i in range(1, amount) if given[i] < most]
        whole, budget = sum([loads[i] for i in movable]), rest
        for i in movable:
            addition = min(most - given[i], max(1, budget * loads[i] // whole), rest)
            given[i] = given[i] + addition
            rest = rest - addition
    return np.array(given)


def gaussian(rng, extent, deviation, reach, cuts=(), kind=jnp.bfloat16):
    values = jax.random.normal(rng, extent, jnp.float32) * deviation
    if len(cuts) > 0:
        values = block_scale(rng, extent, cuts, -0.22, 0.18) * values
    return jnp.clip(values, min=-reach, max=reach).astype(kind)


def setup_inputs(seed: int = 0) -> dict:
    arg_keys = jax.random.split(jax.random.key(seed), 13)
    queries = draw_queries(jax.random.fold_in(arg_keys[12], 71), 0)
    keys = draw_keys(jax.random.fold_in(arg_keys[12], 71), 0)
    values = gaussian(arg_keys[2], (LEN, KV_HEADS * VDIM), 1.0, 6.0, ((0, 32), (1, 4)))
    head_lambda = jnp.clip(0.3 + 0.5 * jax.random.uniform(arg_keys[3], (HEADS,), jnp.float32) ** block_scale(arg_keys[3], (HEADS,), ((0, 4),), -0.2, 0.2), 0.3, 0.8)
    out_gain = jnp.clip(1.0 + 0.18 * jax.random.normal(arg_keys[4], (VDIM,), jnp.float32), 0.1, 1.9)
    expert_input = gaussian(arg_keys[5], (TOKENS, D), 1.0, 6.0, ((0, 128),))
    routes_keys = jax.random.split(jax.random.fold_in(arg_keys[6], 1), TOKENS // TOK_DEV)
    routes_turns = jax.random.permutation(jax.random.fold_in(arg_keys[6], 3), TOKENS // TOK_DEV)
    routes = jax.vmap(lambda own, number: assign_block(jax.random.fold_in(arg_keys[6], 2), own, number, TOK_DEV, EXPERTS, TOPK, CAP, 2))(routes_keys, routes_turns).reshape((TOKENS, TOPK))
    route_weight = jnp.clip(0.2 + 0.400000021 * jax.random.uniform(arg_keys[7], (TOKENS, TOPK), jnp.float32) ** block_scale(arg_keys[7], (TOKENS, TOPK), ((0, 128),), -0.2, 0.2), 0.2, 0.6)
    moe_gain = jnp.clip(1.0 + 0.18 * jax.random.normal(arg_keys[8], (D,), jnp.float32), 0.1, 1.9)
    gate_weight = gaussian(arg_keys[9], (EXPERTS, D, FF), (D // 6) ** -0.5, 0.3125, ((0, 32), (2, 4)))
    up_weight = gaussian(arg_keys[10], (EXPERTS, D, FF), (D // 6) ** -0.5, 0.3125, ((0, 32), (2, 4)))
    down_weight = gaussian(arg_keys[11], (EXPERTS, FF, D), (FF * 16) ** -0.5, 0.03125, ((0, 32), (1, 4)))
    return dict(queries=queries, keys=keys, values=values, head_lambda=head_lambda, out_gain=out_gain, expert_input=expert_input, routes=routes, route_weight=route_weight, moe_gain=moe_gain, gate_weight=gate_weight, up_weight=up_weight, down_weight=down_weight)


epsilon = 1e-05

def attention(queries, keys, values, head_lambda, out_gain):
    group_size = HEADS // KV_HEADS
    block_len = math.gcd(LEN, 512)
    score_scale = HEAD ** (-0.5)
    positions = jnp.arange(LEN, dtype=jnp.int32)

    def one_head(head_index):
        kv_index = head_index // group_size
        head_queries = lax.dynamic_slice_in_dim(queries, head_index * (2 * HEAD), 2 * HEAD, 1).reshape(LEN, 2, HEAD).astype(jnp.float32)
        head_keys = lax.dynamic_slice_in_dim(keys, kv_index * (2 * HEAD), 2 * HEAD, 1).reshape(LEN, 2, HEAD).astype(jnp.float32)
        head_values = lax.dynamic_slice_in_dim(values, kv_index * VDIM, VDIM, 1).astype(jnp.float32)
        weight_lambda = head_lambda[head_index]

        def one_block(block_index):
            query_block = lax.dynamic_slice_in_dim(head_queries, block_index * block_len, block_len, 0)
            scores = jnp.einsum('tmd,smd->mts', query_block, head_keys) * score_scale
            query_pos = block_index * block_len + jnp.arange(block_len, dtype=jnp.int32)
            allowed = (positions[None, :] <= query_pos[:, None])[None]
            masked = jnp.where(allowed, scores, -jnp.inf)
            row_max = lax.optimization_barrier(jnp.max(masked, axis=-1, keepdims=True))
            weights = jnp.where(allowed, jnp.exp(scores - row_max), 0.0)
            totals = lax.optimization_barrier(jnp.sum(weights, axis=-1))
            rounded = lax.optimization_barrier(weights.astype(jnp.bfloat16))
            summed = jnp.einsum('mts,sv->mtv', rounded.astype(jnp.float32), head_values)
            return summed[0] / totals[0][:, None] - weight_lambda * summed[1] / totals[1][:, None]
        return lax.map(one_block, jnp.arange(LEN // block_len, dtype=jnp.int32)).reshape(LEN, VDIM)
    combined = lax.map(one_head, jnp.arange(HEADS, dtype=jnp.int32))
    inverse_rms = lax.rsqrt(lax.optimization_barrier(jnp.mean(combined * combined, axis=-1, keepdims=True)) + epsilon)
    mixed_out = (combined * inverse_rms * out_gain).astype(jnp.bfloat16)
    return jnp.transpose(mixed_out, (1, 0, 2)).reshape(LEN, HEADS * VDIM)

def experts_part(expert_input, routes, route_weight, moe_gain, gate_weight, up_weight, down_weight):
    most_rows = N_EP * N_TP * CAP
    hidden_block = FF // N_TP
    inputs_f32 = expert_input.astype(jnp.float32)
    normed = (inputs_f32 * lax.rsqrt(lax.optimization_barrier(jnp.mean(inputs_f32 * inputs_f32, axis=-1, keepdims=True)) + epsilon) * moe_gain).astype(jnp.bfloat16)
    flat_routes = routes.reshape(-1)
    flat_weights = route_weight.reshape(-1)

    def one_expert(totals, expert_index):
        matches = flat_routes == expert_index
        chosen = jnp.nonzero(matches, size=most_rows, fill_value=0)[0].astype(jnp.int32)
        live_rows = (jnp.arange(most_rows, dtype=jnp.int32) < jnp.sum(matches.astype(jnp.int32))).astype(jnp.float32)
        token_rows = chosen // TOPK
        rows_in = normed[token_rows]
        gate_pre = jnp.dot(rows_in, gate_weight[expert_index], preferred_element_type=jnp.float32)
        up_pre = jnp.dot(rows_in, up_weight[expert_index], preferred_element_type=jnp.float32)
        clipped = jnp.minimum(gate_pre, 7.0)
        up_clip = jnp.clip(up_pre, -7.0, 7.0)
        activation = ((up_clip + 1.0) * clipped * jax.nn.sigmoid(1.702 * clipped)).astype(jnp.bfloat16)
        partial_value = jnp.einsum('rnf,nfd->nrd', activation.reshape(most_rows, N_TP, hidden_block).astype(jnp.float32), down_weight[expert_index].reshape(N_TP, hidden_block, D).astype(jnp.float32))
        rounded = lax.optimization_barrier(partial_value.astype(jnp.bfloat16)).astype(jnp.float32)
        expert_out = lax.optimization_barrier(jnp.sum(rounded, axis=0)).astype(jnp.bfloat16)
        contribution = expert_out.astype(jnp.float32) * (flat_weights[chosen] * live_rows)[:, None]
        return (totals.at[token_rows].add(contribution), None)
    totals, unused = lax.scan(one_expert, jnp.zeros((TOKENS, D), jnp.float32), jnp.arange(EXPERTS, dtype=jnp.int32))
    return totals.astype(jnp.bfloat16)

def reference(queries, keys, values, head_lambda, out_gain, expert_input, routes, route_weight, moe_gain, gate_weight, up_weight, down_weight):
    mixed_out = attention(queries, keys, values, head_lambda, out_gain)
    expert_mix = experts_part(expert_input, routes, route_weight, moe_gain, gate_weight, up_weight, down_weight)
    return (mixed_out, expert_mix)
```

```python
import functools

import jax
import jax.numpy as jnp
from jax import lax
from jax.experimental import pallas as pl
from jax.experimental.pallas import tpu as pltpu
from jax.sharding import PartitionSpec as P

HEADS = 8
KV_HEADS = 4
HEAD = 64
VDIM = 128
LOG2E = 1.4426950408889634
KEY_BLOCK = 1024
CHUNKS = ((0, 4), (4, 8), (12, 8))

epsilon = 1e-05


def attention_kernel(start_ref, lambda_ref, gain_ref, query_ref, key_ref, value_ref, out_ref, max_ref, sum_ref):
    group = pl.program_id(0)
    start = start_ref[group]
    rows = query_ref.shape[1]
    lane = lax.broadcasted_iota(jnp.int32, (rows, 2 * HEAD), 1)
    max_ref[...] = jnp.full(max_ref.shape, -1e30, jnp.float32)
    sum_ref[...] = jnp.zeros(sum_ref.shape, jnp.float32)
    ones = jnp.ones((KEY_BLOCK, VDIM), jnp.bfloat16)

    def one_block(offset, masked):
        keys = key_ref[pl.ds(offset, KEY_BLOCK), :]
        values = jnp.concatenate([value_ref[pl.ds(offset, KEY_BLOCK), :], ones], axis=1)
        if masked:
            column = lax.broadcasted_iota(jnp.int32, (rows, KEY_BLOCK), 1) + offset
            row = lax.broadcasted_iota(jnp.int32, (rows, KEY_BLOCK), 0) + start
            allowed = column <= row
        for which in range(4):
            mapped, head = which // 2, which % 2
            query = query_ref[0, :, head * 2 * HEAD:(head + 1) * 2 * HEAD]
            query = jnp.where((lane // HEAD) == mapped, query, jnp.zeros((), jnp.bfloat16)) * jnp.bfloat16(HEAD ** -0.5)
            scores = lax.dot_general(query, keys, (((1,), (1,)), ((), ())), preferred_element_type=jnp.float32)
            if masked:
                scores = jnp.where(allowed, scores, -1e30)
            old_max = max_ref[which]
            new_max = jnp.maximum(old_max, jnp.max(scores, axis=-1, keepdims=True))
            factor = jnp.exp2((old_max - new_max) * LOG2E)
            weights = jnp.exp2((scores - new_max) * LOG2E).astype(jnp.bfloat16)
            summed = jnp.dot(weights, values, preferred_element_type=jnp.float32)
            sum_ref[which] = factor * sum_ref[which] + summed
            max_ref[which] = new_max

    whole = start // KEY_BLOCK

    def step(index, carry):
        one_block(pl.multiple_of(index * KEY_BLOCK, KEY_BLOCK), False)
        return carry

    lax.fori_loop(0, whole, step, 0)
    one_block(pl.multiple_of(whole * KEY_BLOCK, KEY_BLOCK), True)
    for head in range(2):
        first, second = sum_ref[head], sum_ref[2 + head]
        combined = first[:, :VDIM] / first[:, VDIM:] - lambda_ref[head] * (second[:, :VDIM] / second[:, VDIM:])
        inverse = lax.rsqrt(jnp.mean(combined * combined, axis=-1, keepdims=True) + epsilon)
        out_ref[0, :, head * VDIM:(head + 1) * VDIM] = (combined * inverse * gain_ref[...]).astype(jnp.bfloat16)


def attention(starts, head_lambda, out_gain, query_sets, keys, values):
    groups, rows, width = query_sets.shape
    length = keys.shape[0]
    return pl.pallas_call(
        attention_kernel,
        grid=(groups,),
        in_specs=[
            pl.BlockSpec(memory_space=pltpu.SMEM),
            pl.BlockSpec(memory_space=pltpu.SMEM),
            pl.BlockSpec((1, VDIM), lambda g: (0, 0)),
            pl.BlockSpec((1, rows, width), lambda g: (g, 0, 0)),
            pl.BlockSpec((length, 2 * HEAD), lambda g: (0, 0)),
            pl.BlockSpec((length, VDIM), lambda g: (0, 0)),
        ],
        out_specs=pl.BlockSpec((1, rows, width), lambda g: (g, 0, 0)),
        out_shape=jax.ShapeDtypeStruct((groups, rows, width), jnp.bfloat16),
        scratch_shapes=[
            pltpu.VMEM((4, rows, 1), jnp.float32),
            pltpu.VMEM((4, rows, 2 * VDIM), jnp.float32),
        ],
        compiler_params=pltpu.CompilerParams(vmem_limit_bytes=48 * 1024 * 1024),
        cost_estimate=pl.CostEstimate(flops=18_000_000_000, transcendentals=18_000_000, bytes_accessed=9_000_000),
        name="attention",
    )(starts, head_lambda, out_gain, query_sets, keys, values)


def dispatch_kernel(routes_ref, input_ref, gain_ref, *out_refs):
    tokens = input_ref.shape[0]
    values = input_ref[...].astype(jnp.float32)
    inverse = lax.rsqrt(jnp.mean(values * values, axis=-1, keepdims=True) + epsilon)
    normed = (values * inverse * gain_ref[...]).astype(jnp.bfloat16)
    expert = lax.broadcasted_iota(jnp.int32, (tokens, tokens), 0)
    other = lax.broadcasted_iota(jnp.int32, (tokens, tokens), 1)
    chosen = jnp.zeros((tokens, tokens), jnp.float32)
    for k in range(routes_ref.shape[0]):
        chosen = chosen + jnp.where(routes_ref[k:k + 1, :] == expert, 1.0, 0.0)
    before = jnp.where(expert < other, 1.0, 0.0).astype(jnp.bfloat16)
    rank = jnp.dot(chosen.astype(jnp.bfloat16), before, preferred_element_type=jnp.float32)
    rank = jnp.where(chosen > 0.5, rank, -1.0).astype(jnp.bfloat16)
    for out_ref, (first, count) in zip(out_refs, CHUNKS):
        slots = out_ref.shape[0]
        slot = lax.broadcasted_iota(jnp.int32, (slots, tokens), 0)
        column = lax.broadcasted_iota(jnp.int32, (slots, tokens), 1)
        spread = jnp.where(slot // count == column, 1.0, 0.0).astype(jnp.bfloat16)
        ranks = jnp.dot(spread, rank, preferred_element_type=jnp.float32)
        wanted = (slot % count + first).astype(jnp.float32)
        pick = jnp.where(ranks == wanted, 1.0, 0.0).astype(jnp.bfloat16)
        out_ref[...] = jnp.dot(pick, normed, preferred_element_type=jnp.float32).astype(jnp.bfloat16)


def dispatch(routes, expert_input, moe_gain, experts):
    return pl.pallas_call(
        dispatch_kernel,
        out_shape=[
            jax.ShapeDtypeStruct((experts * count, expert_input.shape[1]), jnp.bfloat16) for unused, count in CHUNKS
        ],
        name="dispatch",
    )(routes.T, expert_input, moe_gain.reshape(1, -1))


def combine_kernel(routes_ref, weight_ref, *refs, chunks, carried):
    out_ref = refs[-1]
    tokens = routes_ref.shape[0]
    row = lax.broadcasted_iota(jnp.int32, (tokens, tokens), 0)
    expert = lax.broadcasted_iota(jnp.int32, (tokens, tokens), 1)
    chosen = jnp.zeros((tokens, tokens), jnp.float32)
    scale = jnp.zeros((tokens, tokens), jnp.float32)
    for k in range(routes_ref.shape[1]):
        match = routes_ref[:, k:k + 1] == expert
        chosen = chosen + jnp.where(match, 1.0, 0.0)
        scale = scale + jnp.where(match, weight_ref[:, k:k + 1], 0.0)
    before = jnp.where(expert < row, 1.0, 0.0).astype(jnp.bfloat16)
    rank = jnp.dot(before, chosen.astype(jnp.bfloat16), preferred_element_type=jnp.float32)
    rank = jnp.where(chosen > 0.5, rank, -1.0).astype(jnp.bfloat16)
    high = scale.astype(jnp.bfloat16)
    low = (scale - high.astype(jnp.float32)).astype(jnp.bfloat16)
    total = refs[len(chunks)][...] if carried else None
    for rows_ref, (first, count) in zip(refs, chunks):
        slots = rows_ref.shape[0]
        slot = lax.broadcasted_iota(jnp.int32, (tokens, slots), 1)
        line = lax.broadcasted_iota(jnp.int32, (tokens, slots), 0)
        spread = jnp.where(slot // count == line, 1.0, 0.0).astype(jnp.bfloat16)
        ranks = jnp.dot(rank, spread, preferred_element_type=jnp.float32)
        here = ranks == (slot % count + first).astype(jnp.float32)
        returned = rows_ref[...]
        for part in (high, low):
            picked = jnp.where(here, jnp.dot(part, spread, preferred_element_type=jnp.float32), 0.0)
            piece = jnp.dot(picked.astype(jnp.bfloat16), returned, preferred_element_type=jnp.float32)
            total = piece if total is None else total + piece
    out_ref[...] = total.astype(out_ref.dtype)


def combine(routes, route_weight, returned, chunks, carried, kind):
    arrays = list(returned) + ([] if carried is None else [carried])
    return pl.pallas_call(
        functools.partial(combine_kernel, chunks=chunks, carried=carried is not None),
        out_shape=jax.ShapeDtypeStruct((routes.shape[0], returned[0].shape[1]), kind),
        name="combine",
    )(routes, route_weight, *arrays)


def expert_rows(rows_in, gate_matrix, up_matrix, down_matrix):
    gate_pre = jnp.dot(rows_in, gate_matrix, preferred_element_type=jnp.float32)
    up_pre = jnp.dot(rows_in, up_matrix, preferred_element_type=jnp.float32)
    clipped = jnp.minimum(gate_pre, 7.0)
    up_clip = jnp.clip(up_pre, -7.0, 7.0)
    activated = ((up_clip + 1.0) * clipped * jax.nn.sigmoid(1.702 * clipped)).astype(jnp.bfloat16)
    return jnp.dot(activated, down_matrix, preferred_element_type=jnp.float32).astype(jnp.bfloat16)


def shards(
    queries,
    keys,
    values,
    head_lambda,
    out_gain,
    expert_input,
    routes,
    route_weight,
    moe_gain,
    gate_weight,
    up_weight,
    down_weight,
):
    ep_count = lax.axis_size("ep")
    me = lax.axis_index("ep")
    partner = ep_count - 1 - me
    half = queries.shape[0] // 2
    swap = [(i, ep_count - 1 - i) for i in range(ep_count)]

    outgoing = dispatch(routes, expert_input, moe_gain, ep_count)
    arrived = [lax.all_to_all(rows, "ep", split_axis=0, concat_axis=0, tiled=True) for rows in outgoing]
    gathered = [lax.all_gather(rows, "tp", axis=0, tiled=True) for rows in arrived]

    other_queries = lax.ppermute(queries[half:], "ep", swap)
    both = jnp.concatenate([keys, values], axis=1)
    both = lax.all_gather(both, "ep", axis=0, tiled=True)
    starts = jnp.stack([2 * half * me, 2 * half * partner + half]).astype(jnp.int32)
    mixed = attention(
        starts,
        head_lambda,
        out_gain.reshape(1, -1),
        jnp.stack([queries[:half], other_queries]),
        both[:, :2 * HEAD],
        both[:, 2 * HEAD:],
    )
    mixed_out = jnp.concatenate([mixed[0], lax.ppermute(mixed[1], "ep", swap)], axis=0)

    partial = [expert_rows(rows, gate_weight[0], up_weight[0], down_weight[0]) for rows in gathered]
    summed = [lax.psum_scatter(rows, "tp", scatter_dimension=0, tiled=True) for rows in partial]
    returned = [lax.all_to_all(rows, "ep", split_axis=0, concat_axis=0, tiled=True) for rows in summed]
    early = combine(routes, route_weight, returned[1:], CHUNKS[1:], None, jnp.float32)
    expert_mix = combine(routes, route_weight, returned[:1], CHUNKS[:1], early, jnp.bfloat16)
    return (mixed_out, expert_mix)


def solution(mesh):
    placed = (
        P("ep", "tp"),
        P("ep", "tp"),
        P("ep", "tp"),
        P("tp"),
        P(),
        P(("ep", "tp"), None),
        P(("ep", "tp"), None),
        P(("ep", "tp"), None),
        P(),
        P("ep", None, "tp"),
        P("ep", None, "tp"),
        P("ep", "tp", None),
    )
    return jax.shard_map(
        shards,
        mesh=mesh,
        in_specs=placed,
        out_specs=(P("ep", "tp"), P(("ep", "tp"), None)),
        check_vma=False,
    )
```

```python
import functools

import jax
import jax.numpy as jnp
from jax import lax
from jax.experimental import pallas as pl
from jax.experimental.pallas import tpu as pltpu
from jax.sharding import PartitionSpec as P


HEAD = 64
VDIM = 128
LOG2E = 1.4426950408889634
KEY_BLOCK = 1024
CHUNKS = ((0, 8), (8, 8), (16, 4))
FAR_STEP = (1, -1, -1)

epsilon = 1e-05


def attention_kernel(start_ref, lambda_ref, gain_ref, query_ref, key_value_ref, out_ref, max_ref, sum_ref):
    start = start_ref[pl.program_id(0)]
    rows = query_ref.shape[1]
    lane = lax.broadcasted_iota(jnp.int32, (rows, 2 * HEAD), 1)
    max_ref[...] = jnp.full(max_ref.shape, -1e30, jnp.float32)
    sum_ref[...] = jnp.zeros(sum_ref.shape, jnp.float32)
    ones = jnp.ones((KEY_BLOCK, VDIM), jnp.bfloat16)

    def one_block(offset, masked):
        keys = key_value_ref[pl.ds(offset, KEY_BLOCK), :2 * HEAD]
        values = jnp.concatenate([key_value_ref[pl.ds(offset, KEY_BLOCK), 2 * HEAD:], ones], axis=1)
        if masked:
            column = lax.broadcasted_iota(jnp.int32, (rows, KEY_BLOCK), 1) + offset
            row = lax.broadcasted_iota(jnp.int32, (rows, KEY_BLOCK), 0) + start
            allowed = column <= row
        for which in range(4):
            mapped, head = which // 2, which % 2
            query = query_ref[0, :, head * 2 * HEAD:(head + 1) * 2 * HEAD]
            query = jnp.where((lane // HEAD) == mapped, query, jnp.zeros((), jnp.bfloat16)) * jnp.bfloat16(HEAD ** -0.5)
            scores = lax.dot_general(query, keys, (((1,), (1,)), ((), ())), preferred_element_type=jnp.float32)
            if masked:
                scores = jnp.where(allowed, scores, -1e30)
            old_max = max_ref[which]
            new_max = jnp.maximum(old_max, jnp.max(scores, axis=-1, keepdims=True))
            factor = jnp.exp2((old_max - new_max) * LOG2E)
            weights = jnp.exp2((scores - new_max) * LOG2E).astype(jnp.bfloat16)
            summed = jnp.dot(weights, values, preferred_element_type=jnp.float32)
            sum_ref[which] = factor * sum_ref[which] + summed
            max_ref[which] = new_max

    whole = start // KEY_BLOCK

    def step(index, carry):
        one_block(pl.multiple_of(index * KEY_BLOCK, KEY_BLOCK), False)
        return carry

    lax.fori_loop(0, whole, step, 0)
    one_block(pl.multiple_of(whole * KEY_BLOCK, KEY_BLOCK), True)
    for head in range(2):
        first, second = sum_ref[head], sum_ref[2 + head]
        combined = first[:, :VDIM] / first[:, VDIM:] - lambda_ref[head] * (second[:, :VDIM] / second[:, VDIM:])
        inverse = lax.rsqrt(jnp.mean(combined * combined, axis=-1, keepdims=True) + epsilon)
        out_ref[0, :, head * VDIM:(head + 1) * VDIM] = (combined * inverse * gain_ref[...]).astype(jnp.bfloat16)


def attention(starts, head_lambda, out_gain, query_sets, keys_values):
    groups, rows, width = query_sets.shape
    length, both = keys_values.shape
    return pl.pallas_call(
        attention_kernel,
        grid=(groups,),
        in_specs=[
            pl.BlockSpec(memory_space=pltpu.SMEM),
            pl.BlockSpec(memory_space=pltpu.SMEM),
            pl.BlockSpec((1, VDIM), lambda g: (0, 0)),
            pl.BlockSpec((1, rows, width), lambda g: (g, 0, 0)),
            pl.BlockSpec((length, both), lambda g: (0, 0)),
        ],
        out_specs=pl.BlockSpec((1, rows, width), lambda g: (g, 0, 0)),
        out_shape=jax.ShapeDtypeStruct((groups, rows, width), jnp.bfloat16),
        scratch_shapes=[
            pltpu.VMEM((4, rows, 1), jnp.float32),
            pltpu.VMEM((4, rows, 2 * VDIM), jnp.float32),
        ],
        compiler_params=pltpu.CompilerParams(vmem_limit_bytes=60 * 1024 * 1024),
        cost_estimate=pl.CostEstimate(flops=18_000_000_000, transcendentals=18_000_000, bytes_accessed=9_000_000),
        name="attention",
    )(starts, head_lambda, out_gain, query_sets, keys_values)


def dispatch_kernel(routes_ref, input_ref, gain_ref, *out_refs):
    tokens = input_ref.shape[0]
    values = input_ref[...].astype(jnp.float32)
    inverse = lax.rsqrt(jnp.mean(values * values, axis=-1, keepdims=True) + epsilon)
    normed = (values * inverse * gain_ref[...]).astype(jnp.bfloat16)
    expert = lax.broadcasted_iota(jnp.int32, (tokens, tokens), 0)
    other = lax.broadcasted_iota(jnp.int32, (tokens, tokens), 1)
    chosen = jnp.zeros((tokens, tokens), jnp.float32)
    for k in range(routes_ref.shape[0]):
        chosen = chosen + jnp.where(routes_ref[k:k + 1, :] == expert, 1.0, 0.0)
    before = jnp.where(expert < other, 1.0, 0.0).astype(jnp.bfloat16)
    rank = jnp.dot(chosen.astype(jnp.bfloat16), before, preferred_element_type=jnp.float32)
    rank = jnp.where(chosen > 0.5, rank, -1.0).astype(jnp.bfloat16)
    for out_ref, (first, count) in zip(out_refs, CHUNKS):
        slots = out_ref.shape[0]
        slot = lax.broadcasted_iota(jnp.int32, (slots, tokens), 0)
        column = lax.broadcasted_iota(jnp.int32, (slots, tokens), 1)
        spread = jnp.where(slot // count == column, 1.0, 0.0).astype(jnp.bfloat16)
        ranks = jnp.dot(spread, rank, preferred_element_type=jnp.float32)
        wanted = (slot % count + first).astype(jnp.float32)
        pick = jnp.where(ranks == wanted, 1.0, 0.0).astype(jnp.bfloat16)
        out_ref[...] = jnp.dot(pick, normed, preferred_element_type=jnp.float32).astype(jnp.bfloat16)


def dispatch(routes, expert_input, moe_gain, experts):
    return pl.pallas_call(
        dispatch_kernel,
        out_shape=[
            jax.ShapeDtypeStruct((experts * count, expert_input.shape[1]), jnp.bfloat16) for unused, count in CHUNKS
        ],
        name="dispatch",
    )(routes.T, expert_input, moe_gain.reshape(1, -1))


def combine_kernel(routes_ref, weight_ref, *refs, chunks, carried):
    out_ref = refs[-1]
    tokens = routes_ref.shape[0]
    row = lax.broadcasted_iota(jnp.int32, (tokens, tokens), 0)
    expert = lax.broadcasted_iota(jnp.int32, (tokens, tokens), 1)
    chosen = jnp.zeros((tokens, tokens), jnp.float32)
    scale = jnp.zeros((tokens, tokens), jnp.float32)
    for k in range(routes_ref.shape[1]):
        match = routes_ref[:, k:k + 1] == expert
        chosen = chosen + jnp.where(match, 1.0, 0.0)
        scale = scale + jnp.where(match, weight_ref[:, k:k + 1], 0.0)
    before = jnp.where(expert < row, 1.0, 0.0).astype(jnp.bfloat16)
    rank = jnp.dot(before, chosen.astype(jnp.bfloat16), preferred_element_type=jnp.float32)
    rank = jnp.where(chosen > 0.5, rank, -1.0).astype(jnp.bfloat16)
    high = scale.astype(jnp.bfloat16)
    low = (scale - high.astype(jnp.float32)).astype(jnp.bfloat16)
    total = refs[len(chunks)][...] if carried else None
    for rows_ref, (first, count) in zip(refs, chunks):
        slots = rows_ref.shape[0]
        slot = lax.broadcasted_iota(jnp.int32, (tokens, slots), 1)
        line = lax.broadcasted_iota(jnp.int32, (tokens, slots), 0)
        spread = jnp.where(slot // count == line, 1.0, 0.0).astype(jnp.bfloat16)
        ranks = jnp.dot(rank, spread, preferred_element_type=jnp.float32)
        here = ranks == (slot % count + first).astype(jnp.float32)
        returned = rows_ref[...]
        for part in (high, low):
            picked = jnp.where(here, jnp.dot(part, spread, preferred_element_type=jnp.float32), 0.0)
            piece = jnp.dot(picked.astype(jnp.bfloat16), returned, preferred_element_type=jnp.float32)
            total = piece if total is None else total + piece
    out_ref[...] = total.astype(out_ref.dtype)


def combine(routes, route_weight, returned, chunks, carried, kind):
    arrays = list(returned) + ([] if carried is None else [carried])
    return pl.pallas_call(
        functools.partial(combine_kernel, chunks=chunks, carried=carried is not None),
        out_shape=jax.ShapeDtypeStruct((routes.shape[0], returned[0].shape[1]), kind),
        name="combine",
    )(routes, route_weight, *arrays)


def expert_kernel(gate_hbm, up_hbm, down_hbm, *refs, sizes, addends):
    count, extra = len(sizes), sum(addends)
    row_hbm, extra_hbm, out_hbm = refs[:count], refs[count:count + extra], refs[count + extra:2 * count + extra]
    gate_ref, up_ref, down_ref, row_ref, out_ref, gate_sem, up_sem, down_sem, row_sem, out_sem = refs[2 * count + extra:][:10]
    extra_refs = refs[2 * count + extra + 10:]
    extra_loads = [
        pltpu.make_async_copy(extra_hbm[i], extra_refs[i], extra_refs[extra].at[i]) for i in range(extra)
    ]
    begins = [sum(sizes[:i]) for i in range(count)]
    loads = [
        pltpu.make_async_copy(row_hbm[i], row_ref.at[pl.ds(begins[i], sizes[i]), :], row_sem.at[i]) for i in range(count)
    ]
    gate_load = pltpu.make_async_copy(gate_hbm, gate_ref, gate_sem)
    up_load = pltpu.make_async_copy(up_hbm, up_ref, up_sem)
    down_load = pltpu.make_async_copy(down_hbm, down_ref, down_sem)
    loads[0].start()
    gate_load.start()
    up_load.start()
    down_load.start()
    for load in loads[1:]:
        load.start()
    for load in extra_loads:
        load.start()
    stores = []
    used = 0
    for i in range(count):
        loads[i].wait()
        rows = row_ref[pl.ds(begins[i], sizes[i]), :]
        if i == 0:
            gate_load.wait()
        gate_pre = jnp.dot(rows, gate_ref[...], preferred_element_type=jnp.float32)
        if i == 0:
            up_load.wait()
        up_pre = jnp.dot(rows, up_ref[...], preferred_element_type=jnp.float32)
        clipped = jnp.minimum(gate_pre, 7.0)
        up_clip = jnp.clip(up_pre, -7.0, 7.0)
        activated = ((up_clip + 1.0) * clipped * jax.nn.sigmoid(1.702 * clipped)).astype(jnp.bfloat16)
        if i == 0:
            down_load.wait()
        partial = jnp.dot(activated, down_ref[...], preferred_element_type=jnp.float32)
        for j in range(used, used + addends[i]):
            extra_loads[j].wait()
            partial = partial + extra_refs[j][...].astype(jnp.float32)
        used += addends[i]
        out_ref[pl.ds(begins[i], sizes[i]), :] = partial.astype(jnp.bfloat16)
        store = pltpu.make_async_copy(out_ref.at[pl.ds(begins[i], sizes[i]), :], out_hbm[i], out_sem.at[i])
        store.start()
        stores.append(store)
    for store in stores:
        store.wait()


def expert(rows, weights, addends):
    width, hidden = weights[0].shape
    sizes = tuple(r.shape[0] for r in rows)
    total = sum(sizes)
    extra = [a for more in addends for a in more]
    return pl.pallas_call(
        functools.partial(expert_kernel, sizes=sizes, addends=tuple(len(more) for more in addends)),
        in_specs=[pl.BlockSpec(memory_space=pltpu.HBM)] * (3 + len(rows) + len(extra)),
        out_specs=[pl.BlockSpec(memory_space=pltpu.HBM)] * len(rows),
        out_shape=[jax.ShapeDtypeStruct(r.shape, jnp.bfloat16) for r in rows],
        scratch_shapes=[
            pltpu.VMEM((width, hidden), jnp.bfloat16),
            pltpu.VMEM((width, hidden), jnp.bfloat16),
            pltpu.VMEM((hidden, width), jnp.bfloat16),
            pltpu.VMEM((total, width), jnp.bfloat16),
            pltpu.VMEM((total, width), jnp.bfloat16),
            pltpu.SemaphoreType.DMA,
            pltpu.SemaphoreType.DMA,
            pltpu.SemaphoreType.DMA,
            pltpu.SemaphoreType.DMA((len(rows),)),
            pltpu.SemaphoreType.DMA((len(rows),)),
        ]
        + [pltpu.VMEM(a.shape, jnp.bfloat16) for a in extra]
        + ([pltpu.SemaphoreType.DMA((len(extra),))] if extra else []),
        compiler_params=pltpu.CompilerParams(vmem_limit_bytes=60 * 1024 * 1024),
        cost_estimate=pl.CostEstimate(
            flops=6 * total * width * hidden, transcendentals=total * hidden, bytes_accessed=6 * width * hidden
        ),
        name="expert",
    )(*weights, *rows, *extra)


def send(value, step):
    size = lax.axis_size("tp")
    return lax.ppermute(value, "tp", [(i, (i + step) % size) for i in range(size)])


def swap_ends(value):
    size = lax.axis_size("ep")
    return lax.ppermute(value, "ep", [(i, size - 1 - i) for i in range(size)])


def exchange(value):
    return lax.all_to_all(value, "ep", split_axis=0, concat_axis=0, tiled=True)


def body(
    queries,
    keys,
    values,
    head_lambda,
    out_gain,
    expert_input,
    routes,
    route_weight,
    moe_gain,
    gate_weight,
    up_weight,
    down_weight,
):
    ep_count = lax.axis_size("ep")
    me = lax.axis_index("ep")
    partner = ep_count - 1 - me
    half = queries.shape[0] // 2

    weights = tuple(
        pltpu.with_memory_space_constraint(w[0], pltpu.HBM) for w in (gate_weight, up_weight, down_weight)
    )

    other_queries = swap_ends(queries[half:])
    outgoing = dispatch(routes, expert_input, moe_gain, ep_count)

    gathered = []
    for name, rows, way in zip("abc", outgoing, FAR_STEP):
        mine = exchange(rows)
        if name == "b":
            keys, values, mine = lax.optimization_barrier((keys, values, mine))
            both = jnp.concatenate([keys, values], axis=1)
            both = lax.all_gather(both, "ep", axis=0, tiled=True)
        behind = send(mine, way)
        ahead = send(mine, -way)
        far = send(behind, way)
        gathered.append((mine, behind, ahead, far))

    starts = jnp.stack([2 * half * me, 2 * half * partner + half]).astype(jnp.int32)
    query_sets = jnp.stack([queries[:half], other_queries])
    mixed = attention(starts, head_lambda, out_gain.reshape(1, -1), query_sets, both)
    mixed_out = jnp.concatenate([mixed[0], swap_ends(mixed[1])], axis=0)

    returned = []
    for (mine, behind, ahead, far), way in zip(gathered, FAR_STEP):
        for_far, for_behind = expert([far, behind], weights, [[], []])
        passing = send(for_far, way)
        from_ahead = send(for_behind, -way)
        (for_ahead,) = expert([ahead], weights, [[passing]])
        from_behind = send(for_ahead, way)
        (own,) = expert([mine], weights, [[from_ahead, from_behind]])
        returned.append(exchange(own))

    early = combine(routes, route_weight, returned[:2], CHUNKS[:2], None, jnp.float32)
    expert_mix = combine(routes, route_weight, returned[2:], CHUNKS[2:], early, jnp.bfloat16)
    return (mixed_out, expert_mix)


def solution(mesh):
    placed = (
        P("ep", "tp"),
        P("ep", "tp"),
        P("ep", "tp"),
        P("tp"),
        P(),
        P(("ep", "tp"), None),
        P(("ep", "tp"), None),
        P(("ep", "tp"), None),
        P(),
        P("ep", None, "tp"),
        P("ep", None, "tp"),
        P("ep", "tp", None),
    )
    return jax.shard_map(
        body,
        mesh=mesh,
        in_specs=placed,
        out_specs=(P("ep", "tp"), P(("ep", "tp"), None)),
        check_vma=False,
    )
```

```python
import functools

import jax
import jax.numpy as jnp
from jax import lax
from jax.experimental import pallas as pl
from jax.experimental.pallas import tpu as pltpu
from jax.sharding import PartitionSpec as P


HEAD = 64
VDIM = 128
LOG2E = 1.4426950408889634
KEY_BLOCK = 1024
SHARE = KEY_BLOCK // 2
CHUNKS = ((0, 8), (8, 8), (16, 4))
GATHER_STEP = (1, -1, -1)

epsilon = 1e-05


def attention_kernel(start_ref, lambda_ref, gain_ref, query_ref, near_key, near_value, side_key, side_value, out_ref, max_ref, sum_ref):
    start = start_ref[pl.program_id(0)]
    rows = query_ref.shape[1]
    lane = lax.broadcasted_iota(jnp.int32, (rows, 2 * HEAD), 1)
    max_ref[...] = jnp.full(max_ref.shape, -1e30, jnp.float32)
    sum_ref[...] = jnp.zeros(sum_ref.shape, jnp.float32)
    ones = jnp.ones((KEY_BLOCK, VDIM), jnp.bfloat16)

    def one_block(offset, masked):
        chip = offset // KEY_BLOCK
        z_off = (chip // 4 + 4 - start_ref[3]) % 4
        y_off = (chip % 4 + 4 - start_ref[4]) % 4
        key_rows = pl.ds(pl.multiple_of((z_off * 4 + y_off) * SHARE, SHARE), SHARE)
        value_rows = pl.ds(pl.multiple_of((y_off * 4 + z_off) * SHARE, SHARE), SHARE)
        keys = jnp.concatenate([near_key[key_rows, :], side_key[key_rows, :]], axis=0)
        values = jnp.concatenate([near_value[value_rows, :], side_value[value_rows, :]], axis=0)
        values = jnp.concatenate([values, ones], axis=1)
        if masked:
            column = lax.broadcasted_iota(jnp.int32, (rows, KEY_BLOCK), 1)
            swapped = jnp.where(column < SHARE, column + SHARE, column - SHARE)
            column = offset + jnp.where(start_ref[2] == 0, column, swapped)
            row = lax.broadcasted_iota(jnp.int32, (rows, KEY_BLOCK), 0) + start
            allowed = column <= row
        for which in range(4):
            mapped, head = which // 2, which % 2
            query = query_ref[0, :, head * 2 * HEAD:(head + 1) * 2 * HEAD]
            query = jnp.where((lane // HEAD) == mapped, query, jnp.zeros((), jnp.bfloat16)) * jnp.bfloat16(HEAD ** -0.5)
            scores = lax.dot_general(query, keys, (((1,), (1,)), ((), ())), preferred_element_type=jnp.float32)
            if masked:
                scores = jnp.where(allowed, scores, -1e30)
            old_max = max_ref[0, which]
            new_max = jnp.maximum(old_max, jnp.max(scores, axis=-1, keepdims=True))
            factor = jnp.exp2((old_max - new_max) * LOG2E)
            weights = jnp.exp2((scores - new_max) * LOG2E).astype(jnp.bfloat16)
            summed = jnp.dot(weights, values, preferred_element_type=jnp.float32)
            sum_ref[0, which] = factor * sum_ref[0, which] + summed
            max_ref[0, which] = new_max

    whole = start // KEY_BLOCK

    def step(index, carry):
        one_block(pl.multiple_of(index * KEY_BLOCK, KEY_BLOCK), False)
        return carry

    lax.fori_loop(0, whole, step, 0)
    one_block(pl.multiple_of(whole * KEY_BLOCK, KEY_BLOCK), True)
    for head in range(2):
        first, second = sum_ref[0, head], sum_ref[0, 2 + head]
        combined = first[:, :VDIM] / first[:, VDIM:] - lambda_ref[head] * (second[:, :VDIM] / second[:, VDIM:])
        inverse = lax.rsqrt(jnp.mean(combined * combined, axis=-1, keepdims=True) + epsilon)
        out_ref[0, :, head * VDIM:(head + 1) * VDIM] = (combined * inverse * gain_ref[...]).astype(jnp.bfloat16)


def attention(starts, head_lambda, out_gain, query_sets, keys_values):
    groups, rows, width = query_sets.shape
    return pl.pallas_call(
        attention_kernel,
        grid=(groups,),
        in_specs=[
            pl.BlockSpec(memory_space=pltpu.SMEM),
            pl.BlockSpec(memory_space=pltpu.SMEM),
            pl.BlockSpec((1, VDIM), lambda g: (0, 0)),
            pl.BlockSpec((1, rows, width), lambda g: (g, 0, 0)),
        ]
        + [pl.BlockSpec(memory_space=pltpu.VMEM)] * 4,
        out_specs=pl.BlockSpec((1, rows, width), lambda g: (g, 0, 0)),
        out_shape=jax.ShapeDtypeStruct((groups, rows, width), jnp.bfloat16),
        scratch_shapes=[pltpu.VMEM((1, 4, rows, 1), jnp.float32), pltpu.VMEM((1, 4, rows, 2 * VDIM), jnp.float32)],
        compiler_params=pltpu.CompilerParams(vmem_limit_bytes=60 * 1024 * 1024),
        cost_estimate=pl.CostEstimate(flops=18_000_000_000, transcendentals=18_000_000, bytes_accessed=9_000_000),
        name="attention",
    )(starts, head_lambda, out_gain, query_sets, *keys_values)


def dispatch_kernel(routes_ref, input_ref, gain_ref, *out_refs):
    tokens = input_ref.shape[0]
    values = input_ref[...].astype(jnp.float32)
    inverse = lax.rsqrt(jnp.mean(values * values, axis=-1, keepdims=True) + epsilon)
    normed = (values * inverse * gain_ref[...]).astype(jnp.bfloat16)
    expert = lax.broadcasted_iota(jnp.int32, (tokens, tokens), 0)
    other = lax.broadcasted_iota(jnp.int32, (tokens, tokens), 1)
    chosen = jnp.zeros((tokens, tokens), jnp.float32)
    for k in range(routes_ref.shape[0]):
        chosen = chosen + jnp.where(routes_ref[k:k + 1, :] == expert, 1.0, 0.0)
    before = jnp.where(expert < other, 1.0, 0.0).astype(jnp.bfloat16)
    rank = jnp.dot(chosen.astype(jnp.bfloat16), before, preferred_element_type=jnp.float32)
    rank = jnp.where(chosen > 0.5, rank, -1.0).astype(jnp.bfloat16)
    for out_ref, (first, count) in zip(out_refs, CHUNKS):
        slots = out_ref.shape[0]
        slot = lax.broadcasted_iota(jnp.int32, (slots, tokens), 0)
        column = lax.broadcasted_iota(jnp.int32, (slots, tokens), 1)
        spread = jnp.where(slot // count == column, 1.0, 0.0).astype(jnp.bfloat16)
        ranks = jnp.dot(spread, rank, preferred_element_type=jnp.float32)
        wanted = (slot % count + first).astype(jnp.float32)
        pick = jnp.where(ranks == wanted, 1.0, 0.0).astype(jnp.bfloat16)
        out_ref[...] = jnp.dot(pick, normed, preferred_element_type=jnp.float32).astype(jnp.bfloat16)


def dispatch(routes, expert_input, moe_gain, experts):
    return pl.pallas_call(
        dispatch_kernel,
        out_shape=[
            jax.ShapeDtypeStruct((experts * count, expert_input.shape[1]), jnp.bfloat16) for unused, count in CHUNKS
        ],
        name="dispatch",
    )(routes.T, expert_input, moe_gain.reshape(1, -1))


def combine_kernel(routes_ref, weight_ref, *refs, chunks, carried):
    out_ref = refs[-1]
    tokens = routes_ref.shape[0]
    row = lax.broadcasted_iota(jnp.int32, (tokens, tokens), 0)
    expert = lax.broadcasted_iota(jnp.int32, (tokens, tokens), 1)
    chosen = jnp.zeros((tokens, tokens), jnp.float32)
    scale = jnp.zeros((tokens, tokens), jnp.float32)
    for k in range(routes_ref.shape[1]):
        match = routes_ref[:, k:k + 1] == expert
        chosen = chosen + jnp.where(match, 1.0, 0.0)
        scale = scale + jnp.where(match, weight_ref[:, k:k + 1], 0.0)
    before = jnp.where(expert < row, 1.0, 0.0).astype(jnp.bfloat16)
    rank = jnp.dot(before, chosen.astype(jnp.bfloat16), preferred_element_type=jnp.float32)
    rank = jnp.where(chosen > 0.5, rank, -1.0).astype(jnp.bfloat16)
    high = scale.astype(jnp.bfloat16)
    low = (scale - high.astype(jnp.float32)).astype(jnp.bfloat16)
    total = refs[len(chunks)][...] if carried else None
    for rows_ref, (first, count) in zip(refs, chunks):
        slots = rows_ref.shape[0]
        slot = lax.broadcasted_iota(jnp.int32, (tokens, slots), 1)
        line = lax.broadcasted_iota(jnp.int32, (tokens, slots), 0)
        spread = jnp.where(slot // count == line, 1.0, 0.0).astype(jnp.bfloat16)
        ranks = jnp.dot(rank, spread, preferred_element_type=jnp.float32)
        here = ranks == (slot % count + first).astype(jnp.float32)
        returned = rows_ref[...]
        for part in (high, low):
            picked = jnp.where(here, jnp.dot(part, spread, preferred_element_type=jnp.float32), 0.0)
            piece = jnp.dot(picked.astype(jnp.bfloat16), returned, preferred_element_type=jnp.float32)
            total = piece if total is None else total + piece
    out_ref[...] = total.astype(out_ref.dtype)


def combine(routes, route_weight, returned, chunks, carried, kind):
    arrays = list(returned) + ([] if carried is None else [carried])
    return pl.pallas_call(
        functools.partial(combine_kernel, chunks=chunks, carried=carried is not None),
        out_shape=jax.ShapeDtypeStruct((routes.shape[0], returned[0].shape[1]), kind),
        name="combine",
    )(routes, route_weight, *arrays)


def expert_kernel(gate_hbm, up_hbm, down_hbm, *refs, sizes, addends):
    count, extra = len(sizes), sum(addends)
    row_hbm, extra_hbm, out_hbm = refs[:count], refs[count:count + extra], refs[count + extra:2 * count + extra]
    gate_ref, up_ref, down_ref, row_ref, out_ref, gate_sem, up_sem, down_sem, row_sem, out_sem = refs[2 * count + extra:][:10]
    extra_refs = refs[2 * count + extra + 10:]
    extra_loads = [
        pltpu.make_async_copy(extra_hbm[i], extra_refs[i], extra_refs[extra].at[i]) for i in range(extra)
    ]
    begins = [sum(sizes[:i]) for i in range(count)]
    loads = [
        pltpu.make_async_copy(row_hbm[i], row_ref.at[pl.ds(begins[i], sizes[i]), :], row_sem.at[i]) for i in range(count)
    ]
    gate_load = pltpu.make_async_copy(gate_hbm, gate_ref, gate_sem)
    up_load = pltpu.make_async_copy(up_hbm, up_ref, up_sem)
    down_load = pltpu.make_async_copy(down_hbm, down_ref, down_sem)
    loads[0].start()
    gate_load.start()
    up_load.start()
    down_load.start()
    for load in loads[1:]:
        load.start()
    for load in extra_loads:
        load.start()
    stores = []
    used = 0
    for i in range(count):
        loads[i].wait()
        if i == 0:
            gate_load.wait()
            up_load.wait()
            down_load.wait()
        mine = range(used, used + addends[i])
        for j in mine:
            extra_loads[j].wait()
        part = sizes[i] // 2

        def half(index, carry, begin=begins[i], part=part, mine=mine):
            here = pl.ds(pl.multiple_of(begin + index * part, part), part)
            rows = row_ref[here, :]
            gate_pre = jnp.dot(rows, gate_ref[...], preferred_element_type=jnp.float32)
            up_pre = jnp.dot(rows, up_ref[...], preferred_element_type=jnp.float32)
            clipped = jnp.minimum(gate_pre, 7.0)
            up_clip = jnp.clip(up_pre, -7.0, 7.0)
            activated = ((up_clip + 1.0) * clipped * jax.nn.sigmoid(1.702 * clipped)).astype(jnp.bfloat16)
            partial = jnp.dot(activated, down_ref[...], preferred_element_type=jnp.float32)
            for j in mine:
                partial = partial + extra_refs[j][pl.ds(pl.multiple_of(index * part, part), part), :].astype(jnp.float32)
            out_ref[here, :] = partial.astype(jnp.bfloat16)
            return carry

        lax.fori_loop(0, 2, half, 0)
        used += addends[i]
        store = pltpu.make_async_copy(out_ref.at[pl.ds(begins[i], sizes[i]), :], out_hbm[i], out_sem.at[i])
        store.start()
        stores.append(store)
    for store in stores:
        store.wait()


def expert(rows, weights, addends):
    width, hidden = weights[0].shape
    sizes = tuple(r.shape[0] for r in rows)
    total = sum(sizes)
    extra = [a for more in addends for a in more]
    return pl.pallas_call(
        functools.partial(expert_kernel, sizes=sizes, addends=tuple(len(more) for more in addends)),
        in_specs=[pl.BlockSpec(memory_space=pltpu.HBM)] * (3 + len(rows) + len(extra)),
        out_specs=[pl.BlockSpec(memory_space=pltpu.HBM)] * len(rows),
        out_shape=[jax.ShapeDtypeStruct(r.shape, jnp.bfloat16) for r in rows],
        scratch_shapes=[
            pltpu.VMEM((width, hidden), jnp.bfloat16),
            pltpu.VMEM((width, hidden), jnp.bfloat16),
            pltpu.VMEM((hidden, width), jnp.bfloat16),
            pltpu.VMEM((total, width), jnp.bfloat16),
            pltpu.VMEM((total, width), jnp.bfloat16),
            pltpu.SemaphoreType.DMA,
            pltpu.SemaphoreType.DMA,
            pltpu.SemaphoreType.DMA,
            pltpu.SemaphoreType.DMA((len(rows),)),
            pltpu.SemaphoreType.DMA((len(rows),)),
        ]
        + [pltpu.VMEM(a.shape, jnp.bfloat16) for a in extra]
        + ([pltpu.SemaphoreType.DMA((len(extra),))] if extra else []),
        compiler_params=pltpu.CompilerParams(vmem_limit_bytes=60 * 1024 * 1024),
        cost_estimate=pl.CostEstimate(
            flops=6 * total * width * hidden, transcendentals=total * hidden, bytes_accessed=6 * width * hidden
        ),
        name="expert",
    )(*weights, *rows, *extra)


def send(value, step):
    size = lax.axis_size("tp")
    return lax.ppermute(value, "tp", [(i, (i + step) % size) for i in range(size)])


def swap_ends(value):
    size = lax.axis_size("ep")
    return lax.ppermute(value, "ep", [(i, size - 1 - i) for i in range(size)])


def around(value, stride):
    size = lax.axis_size("ep")

    def shift(part, step):
        moved = [(i, i + ((i // stride + step) % 4 - i // stride % 4) * stride) for i in range(size)]
        return lax.ppermute(part, "ep", moved)

    behind = shift(value, 1)
    ahead = shift(value, -1)
    far = shift(behind, 1)
    return jnp.concatenate([value, ahead, far, behind], axis=0)


def sibling(value):
    size = lax.axis_size("ep")
    return lax.ppermute(value, "ep", [(i, i + 1 - 2 * (i % 2)) for i in range(size)])


def exchange(value):
    return lax.all_to_all(value, "ep", split_axis=0, concat_axis=0, tiled=True)


def body(
    queries,
    keys,
    values,
    head_lambda,
    out_gain,
    expert_input,
    routes,
    route_weight,
    moe_gain,
    gate_weight,
    up_weight,
    down_weight,
):
    ep_count = lax.axis_size("ep")
    me = lax.axis_index("ep")
    partner = ep_count - 1 - me
    half = queries.shape[0] // 2

    weights = tuple(
        pltpu.with_memory_space_constraint(w[0], pltpu.HBM) for w in (gate_weight, up_weight, down_weight)
    )

    other_queries = swap_ends(queries[half:])
    near_key = around(around(keys, 2), 8)
    near_value = around(around(values, 8), 2)
    both = (near_key, near_value, sibling(near_key), sibling(near_value))
    outgoing = dispatch(routes, expert_input, moe_gain, ep_count)

    gathered = []
    for rows, way in zip(outgoing, GATHER_STEP):
        mine = exchange(rows)
        behind = send(mine, way)
        ahead = send(mine, -way)
        far = send(behind, way)
        gathered.append((mine, behind, ahead, far))

    starts = jnp.stack([2 * half * me, 2 * half * partner + half, me % 2, me // 8, me // 2 % 4]).astype(jnp.int32)
    query_sets = jnp.stack([queries[:half], other_queries])
    mixed = attention(starts, head_lambda, out_gain.reshape(1, -1), query_sets, both)
    mixed_out = jnp.concatenate([mixed[0], swap_ends(mixed[1])], axis=0)

    def call(rows, addends):
        return expert(rows, weights, addends)

    (a_mine, a_behind, a_ahead, a_far), (b_mine, b_behind, b_ahead, b_far), (c_mine, c_behind, c_ahead, c_far) = gathered
    c_behind, c_ahead = c_ahead, c_behind
    way_a, way_b, way_c = 1, -1, 1

    for_far, for_behind = call([a_far, a_behind], [[], []])
    passing_a, a_first = send(for_far, way_a), send(for_behind, -way_a)
    for_far, for_behind = call([b_far, b_behind], [[], []])
    passing_b, b_first = send(for_far, way_b), send(for_behind, -way_b)
    (for_ahead,) = call([a_ahead], [[passing_a]])
    a_second = send(for_ahead, way_a)
    for_ahead, for_far, for_behind = call([b_ahead, c_far, c_behind], [[passing_b], [], []])
    b_second = send(for_ahead, way_b)
    passing_c, c_first = send(for_far, way_c), send(for_behind, -way_c)
    (own_a,) = call([a_mine], [[a_first, a_second]])
    own_b, for_ahead = call([b_mine, c_ahead], [[b_first, b_second], [passing_c]])
    c_second = send(for_ahead, way_c)
    (own_c,) = call([c_mine], [[c_first, c_second]])
    returned = [exchange(own_a), exchange(own_b), exchange(own_c)]

    early = combine(routes, route_weight, returned[:2], CHUNKS[:2], None, jnp.float32)
    expert_mix = combine(routes, route_weight, returned[2:], CHUNKS[2:], early, jnp.bfloat16)
    return (mixed_out, expert_mix)


def solution(mesh):
    placed = (
        P("ep", "tp"),
        P("ep", "tp"),
        P("ep", "tp"),
        P("tp"),
        P(),
        P(("ep", "tp"), None),
        P(("ep", "tp"), None),
        P(("ep", "tp"), None),
        P(),
        P("ep", None, "tp"),
        P("ep", None, "tp"),
        P("ep", "tp", None),
    )
    return jax.shard_map(
        body,
        mesh=mesh,
        in_specs=placed,
        out_specs=(P("ep", "tp"), P(("ep", "tp"), None)),
        check_vma=False,
    )
```
